32 devices in a mesh: sp: 16 (over z, y, x), tp: 2 (over core).
Axes of the slice: x: 2, y: 2, z: 4, core: 2. Of those that a mesh axis runs over, the one named last changes fastest.
Arguments:
- inputs: bfloat16 [4096, 2048], P('sp', 'tp'), may hold values from -200 to 200
- input_gain: bfloat16 [2048], P('tp'), may hold values from 0.099609375 to 1.8984375
- stick_query_w: bfloat16 [2048, 1024], P(None, 'tp'), may hold values from -0.3125 to 0.3125
- stick_key_w: bfloat16 [2048, 1024], P(None, 'tp'), may hold values from -0.125 to 0.125
- stick_value_w: bfloat16 [2048, 1024], P(None, 'tp'), may hold values from -0.125 to 0.125
- ret_query_w: bfloat16 [2048, 2048], P(None, 'tp'), may hold values from -0.125 to 0.125
- ret_key_w: bfloat16 [2048, 2048], P(None, 'tp'), may hold values from -0.125 to 0.125
- ret_value_w: bfloat16 [2048, 2048], P(None, 'tp'), may hold values from -0.125 to 0.125
- stick_offset: float32 [8], P('tp'), may hold values from -17 to -2
- ret_log_decay: float32 [8], P('tp'), may hold values from -0.04 to 0, as said below
- initial_state: float32 [8, 256, 256], P('tp', 'sp'), may hold values from -38.4 to 38.4
- stick_gain: float32 [1024], P('tp'), may hold values from 0.1 to 1.9
- ret_gain: float32 [2048], P('tp'), may hold values from 0.1 to 1.9
- stick_out_w: bfloat16 [1024, 2048], P('tp', 'sp'), may hold values from -0.125 to 0.125
- ret_out_w: bfloat16 [2048, 2048], P('tp', 'sp'), may hold values from -0.09375 to 0.09375
Outputs:
- layer_out: bfloat16 [4096, 2048], P(('sp', 'tp'))
The draws below stay inside these ranges and needn't reach their ends.
Inputs may be any that keep to these rules, and one draw needn't show every extreme that they name: `ret_log_decay`: every entry is negative.
All inputs are finite; a program needn't handle non-finite values.
Results may differ from the reference program's by a relative error of at most 0.017.
Values may be sent and summed in bfloat16 or wider, within the bound.
A program may use at most 128 MiB of HBM per device.

```python
import math
import jax
import jax.numpy as jnp
from jax import lax

D = 2048
STICK_HEADS = 8
STICK_DIM = 128
RET_HEADS = 8
RET_DIM = 256
TOKENS = 4096
N_TP = 2


def draw_inputs(key, part):
    base_key, row_key, col_key = jax.random.split(jax.random.fold_in(key, 11), 3)
    base = jax.random.normal(base_key, (TOKENS, D), jnp.float32)
    position_ramp = jnp.arange(D, dtype=jnp.float32) / D
    roughness = jax.random.uniform(col_key, (D,), jnp.float32, 0.5, 1.5)
    row_scale = jnp.exp(jax.random.uniform(row_key, (TOKENS, 1), jnp.float32, 0.0, 2.3))
    col_scale = 3.0 ** position_ramp * roughness
    values = row_scale * base * col_scale[None, :]
    return jnp.clip(values, -200.0, 200.0).astype(jnp.bfloat16)


def draw_stick_offset(key, part):
    order_key, near_key, far_key = jax.random.split(jax.random.fold_in(key, 23), 3)
    ranking = jax.random.permutation(order_key, STICK_HEADS)
    fast_heads = ranking < STICK_HEADS // 2
    near_offset = -jnp.log(40.0) - 3.1 + jax.random.uniform(near_key, (STICK_HEADS,), jnp.float32, -0.5, 0.5)
    far_offset = -jnp.log(TOKENS * 1.0) - 3.1 - jax.random.uniform(far_key, (STICK_HEADS,), jnp.float32, 0.0, 1.5)
    return jnp.where(fast_heads, near_offset, far_offset).astype(jnp.float32)


def draw_ret_log_decay(key, part):
    order_key, quick_key, slow_key = jax.random.split(jax.random.fold_in(key, 37), 3)
    ranking = jax.random.permutation(order_key, RET_HEADS)
    fast_heads = ranking < RET_HEADS // 2
    quick_decay = -jax.random.uniform(quick_key, (RET_HEADS,), jnp.float32, 0.01, 0.034)
    slow_decay = -jax.random.uniform(slow_key, (RET_HEADS,), jnp.float32, 0.2, 1.5) / TOKENS
    return jnp.where(fast_heads, quick_decay, slow_decay).astype(jnp.float32)


def level_of(rng, extent, pieces, low, largest):
    def one(axis_at, blocks):
        steps = jax.random.uniform(jax.random.fold_in(jax.random.fold_in(rng, 6), axis_at), (blocks,), jnp.float32, low / len(pieces), largest / len(pieces))
        return jnp.repeat(jnp.exp(steps), extent[axis_at] // blocks).reshape((-1,) + (1,) * (len(extent) - axis_at - 1))

    gain = one(*pieces[0])
    for cut in pieces[1:]:
        gain = gain * one(*cut)
    return gain


def bell_draw(key, shape, scale, limit, shards=(), kind=jnp.bfloat16):
    gain = level_of(key, shape, shards, -0.22, 0.18) if shards else 1.0
    values = jax.random.normal(key, shape, jnp.float32) * scale * gain
    return jnp.minimum(jnp.maximum(values, -limit), limit).astype(kind)


def setup_inputs(seed: int = 0) -> dict:
    streams_of = jax.random.split(jax.random.key(seed), 16)
    return {
        "inputs": draw_inputs(jax.random.fold_in(streams_of[15], 71), 0),
        "input_gain": jnp.clip(1.0 + 0.18 * jax.random.normal(streams_of[1], (D,), jnp.float32), 0.099609375, 1.8984375).astype(jnp.bfloat16),
        "stick_query_w": bell_draw(streams_of[2], (D, STICK_HEADS * STICK_DIM), (D // 6) ** -0.5, 0.3125, ((1, 2),)),
        "stick_key_w": bell_draw(streams_of[3], (D, STICK_HEADS * STICK_DIM), D ** -0.5, 0.125, ((1, 2),)),
        "stick_value_w": bell_draw(streams_of[4], (D, STICK_HEADS * STICK_DIM), D ** -0.5, 0.125, ((1, 2),)),
        "ret_query_w": bell_draw(streams_of[5], (D, RET_HEADS * RET_DIM), D ** -0.5, 0.125, ((1, 2),)),
        "ret_key_w": bell_draw(streams_of[6], (D, RET_HEADS * RET_DIM), D ** -0.5, 0.125, ((1, 2),)),
        "ret_value_w": bell_draw(streams_of[7], (D, RET_HEADS * RET_DIM), D ** -0.5, 0.125, ((1, 2),)),
        "stick_offset": draw_stick_offset(jax.random.fold_in(streams_of[15], 71), 0),
        "ret_log_decay": draw_ret_log_decay(jax.random.fold_in(streams_of[15], 71), 0),
        "initial_state": bell_draw(streams_of[10], (RET_HEADS, RET_DIM, RET_DIM), (0.1 * TOKENS ** 0.5), 38.4, ((0, 2), (1, 16)), jnp.float32),
        "stick_gain": jnp.clip(1.0 + 0.18 * jax.random.normal(streams_of[11], (STICK_HEADS * STICK_DIM,), jnp.float32), 0.1, 1.9),
        "ret_gain": jnp.clip(1.0 + 0.18 * jax.random.normal(streams_of[12], (RET_HEADS * RET_DIM,), jnp.float32), 0.1, 1.9),
        "stick_out_w": bell_draw(streams_of[13], (STICK_HEADS * STICK_DIM, D), (2 * STICK_HEADS * STICK_DIM) ** -0.5, 0.125, ((0, 2), (1, 16))),
        "ret_out_w": bell_draw(streams_of[14], (RET_HEADS * RET_DIM, D), (2 * RET_HEADS * RET_DIM) ** -0.5, 0.09375, ((0, 2), (1, 16))),
    }


epsilon = 1e-06
rope_base = 10000.0

def rotate(values, positions):
    half_width = values.shape[-1] // 2
    inverse = rope_base ** (-jnp.arange(half_width, dtype=jnp.float32) / half_width)
    angles = positions.astype(jnp.float32)[:, None] * inverse[None, :]
    cosine = jnp.cos(angles)[:, None, :]
    sine_table = jnp.sin(angles)[:, None, :]
    first_half = values[..., :half_width]
    second_half = values[..., half_width:]
    return jnp.concatenate([first_half * cosine - second_half * sine_table, second_half * cosine + first_half * sine_table], axis=-1)

def stick_head(packed):
    queries, key_table, value_table, offset = packed
    length = queries.shape[0]
    block_len = math.gcd(length, 1024)
    score_scale = queries.shape[1] ** (-0.5)

    def one_block(block_index):
        query_start = block_index * block_len
        query_rows = lax.dynamic_slice_in_dim(queries, query_start, block_len, 0)
        query_pos = query_start + jnp.arange(block_len, dtype=jnp.int32)

        def advance(turn_index, start_carry):
            running, before = start_carry
            key_start = (block_index - turn_index) * block_len
            key_rows = lax.dynamic_slice_in_dim(key_table, key_start, block_len, 0)
            value_rows = lax.dynamic_slice_in_dim(value_table, key_start, block_len, 0)
            key_pos = key_start + jnp.arange(block_len, dtype=jnp.int32)
            scores = jnp.dot(query_rows, key_rows.T, preferred_element_type=jnp.float32) * score_scale + offset
            allowed = key_pos[None, :] < query_pos[:, None]
            remain = jnp.where(allowed, jax.nn.log_sigmoid(-scores), 0.0)
            suffix = lax.cumsum(remain, axis=1, reverse=True) - remain + before[:, None]
            weights = jnp.where(allowed, jnp.exp(jax.nn.log_sigmoid(scores) + suffix), 0.0).astype(jnp.bfloat16)
            running = running + jnp.dot(weights, value_rows, preferred_element_type=jnp.float32)
            return (running, before + lax.optimization_barrier(jnp.sum(remain, axis=1)))
        start_carry = (jnp.zeros((block_len, value_table.shape[1]), jnp.float32), jnp.zeros((block_len,), jnp.float32))
        running, _ = lax.fori_loop(0, block_index + 1, advance, start_carry)
        return running
    return lax.map(one_block, jnp.arange(length // block_len, dtype=jnp.int32))

def retention(queries, key_table, value_table, log_decay, initial_state):
    length, head_count, ret_width = queries.shape
    block_len = math.gcd(length, 256)
    count_blocks = length // block_len
    local_pos = jnp.arange(block_len, dtype=jnp.float32)
    distance = local_pos[:, None] - local_pos[None, :]
    decay_mask = jnp.where(distance[None] >= 0.0, jnp.exp(log_decay[:, None, None] * jnp.maximum(distance, 0.0)[None]), 0.0)
    query_decay = jnp.exp(log_decay[None, :] * (local_pos[:, None] + 1.0))
    key_decay = jnp.exp(log_decay[None, :] * (block_len - 1.0 - local_pos[:, None]))
    block_decay = jnp.exp(log_decay * block_len)
    highest = lax.Precision.HIGHEST

    def advance(carried_state, blocks):
        query_block, key_block, value_block = blocks
        scores = jnp.einsum('thd,shd->hts', query_block, key_block, precision=highest) * decay_mask
        inner_part = jnp.einsum('hts,she->the', scores, value_block, precision=highest)
        cross_part = jnp.einsum('thd,hde->the', query_block, carried_state, precision=highest) * query_decay[:, :, None]
        carried_state = carried_state * block_decay[:, None, None] + jnp.einsum('shd,she->hde', key_block * key_decay[:, :, None], value_block, precision=highest)
        return (carried_state, inner_part + cross_part)
    blocks = tuple((array.reshape(count_blocks, block_len, head_count, ret_width) for array in (queries, key_table, value_table)))
    _, outputs = lax.scan(advance, initial_state, blocks)
    return outputs.reshape(length, head_count, ret_width)

def head_major(array, head_count):
    return jnp.transpose(array.reshape(array.shape[0], head_count, -1), (1, 0, 2))

def reference(inputs, input_gain, stick_query_w, stick_key_w, stick_value_w, ret_query_w, ret_key_w, ret_value_w, stick_offset, ret_log_decay, initial_state, stick_gain, ret_gain, stick_out_w, ret_out_w):
    length = inputs.shape[0]
    widened = inputs.astype(jnp.float32)
    row_scale = lax.rsqrt(lax.optimization_barrier(jnp.mean(widened * widened, axis=1)) + epsilon)
    scaled = (widened * input_gain.astype(jnp.float32)).astype(jnp.bfloat16)

    def project(weight):
        return (jnp.dot(scaled, weight, preferred_element_type=jnp.float32) * row_scale[:, None]).astype(jnp.bfloat16)
    stick_query = project(stick_query_w)
    stick_key = project(stick_key_w)
    stick_value = project(stick_value_w)
    ret_query = project(ret_query_w)
    ret_key = project(ret_key_w)
    ret_value = project(ret_value_w)
    stick_blocks = lax.map(stick_head, (head_major(stick_query, STICK_HEADS), head_major(stick_key, STICK_HEADS), head_major(stick_value, STICK_HEADS), stick_offset))
    stick_total = jnp.transpose(stick_blocks.reshape(STICK_HEADS, length, STICK_DIM), (1, 0, 2)).reshape(length, STICK_HEADS * STICK_DIM)
    stick_scale = lax.rsqrt(lax.optimization_barrier(jnp.mean(stick_total * stick_total, axis=1)) + epsilon)
    stick_normed = (stick_total * stick_scale[:, None] * stick_gain).astype(jnp.bfloat16)
    positions = jnp.arange(length, dtype=jnp.int32)
    turned_query = rotate(ret_query.reshape(length, RET_HEADS, RET_DIM).astype(jnp.float32), positions)
    turned_key = rotate(ret_key.reshape(length, RET_HEADS, RET_DIM).astype(jnp.float32), positions) * RET_DIM ** (-0.5)
    ret_values = ret_value.reshape(length, RET_HEADS, RET_DIM).astype(jnp.float32)
    ret_total = retention(turned_query, turned_key, ret_values, ret_log_decay, initial_state)
    centered = ret_total - lax.optimization_barrier(jnp.mean(ret_total, axis=2, keepdims=True))
    normed = centered * lax.rsqrt(lax.optimization_barrier(jnp.mean(centered * centered, axis=2, keepdims=True)) + epsilon)
    ret_normed = (normed.reshape(length, RET_HEADS * RET_DIM) * ret_gain).astype(jnp.bfloat16)
    stick_share = STICK_HEADS // N_TP * STICK_DIM
    ret_share = RET_HEADS // N_TP * RET_DIM
    layer_sum = jnp.zeros((length, D), jnp.float32)
    for run_index in range(N_TP):
        stick_cols = slice(run_index * stick_share, (run_index + 1) * stick_share)
        ret_cols = slice(run_index * ret_share, (run_index + 1) * ret_share)
        partial_value = jnp.dot(stick_normed[:, stick_cols], stick_out_w[stick_cols], preferred_element_type=jnp.float32)
        partial_value = partial_value + jnp.dot(ret_normed[:, ret_cols], ret_out_w[ret_cols], preferred_element_type=jnp.float32)
        rounded = lax.optimization_barrier(partial_value.astype(jnp.bfloat16))
        layer_sum = layer_sum + rounded.astype(jnp.float32)
    return layer_sum.astype(jnp.bfloat16)
```

```python
import functools
import math

import jax
import jax.numpy as jnp
from jax import lax
from jax.experimental import pallas as pl
from jax.experimental.pallas import tpu as pltpu
from jax.sharding import PartitionSpec as P

D = 2048
STICK_HEADS = 8
STICK_DIM = 128

epsilon = 1e-06
rope_base = 10000.0
MESH = pl.DeviceIdType.MESH
LOG2E = math.log2(math.e)


def mixer_kernel(
    n, heads,
    off_ref, q_ref, k_ref, v_ref, st_ref, init_ref, dec_ref,
    out_ref, ent_ref,
    kbuf, vbuf, qbuf, res, back, sbuf, ebuf, ent,
    k_send, v_send, q_send, r_send, s_send, e_send,
    k_recv, v_recv, q_recv, r_recv, s_recv, e_recv,
):
    me = lax.axis_index("sp")
    group = n // heads
    rows = q_ref.shape[0]
    width = q_ref.shape[1] // heads
    my_head = me // group
    my_slot = lax.rem(me, group)

    def flip(run, place):
        return jnp.where(lax.rem(run, 2) == 0, place, group - 1 - place)

    def columns(head):
        return pl.ds(pl.multiple_of(head * width, width), width)

    def copy(source, target, send, recv, peer):
        return pltpu.make_async_remote_copy(
            src_ref=source, dst_ref=target, send_sem=send, recv_sem=recv,
            device_id={"sp": peer}, device_id_type=MESH,
        )

    def arrived(target, recv):
        copy(target, target, recv, recv, me).wait_recv()

    def sent(source, send):
        copy(source, source, send, send, me).wait_send()

    barrier = pltpu.get_barrier_semaphore()
    for step in range(1, n):
        pl.semaphore_signal(
            barrier, inc=1, device_id={"sp": lax.rem(me + step, n)}, device_id_type=MESH
        )
    pl.semaphore_wait(barrier, n - 1)

    for step in range(1, n):
        peer = lax.rem(me + step, n)
        copy(st_ref.at[peer], sbuf.at[me], s_send.at[peer], s_recv.at[me], peer).start()
    my_run = me // group
    owner_slot = flip(my_run, my_slot)
    for head in range(heads):
        owner = head * group + owner_slot
        part = q_ref.at[:, head * width:(head + 1) * width]

        @pl.when(owner != me)
        def _():
            copy(part, qbuf.at[my_run], q_send.at[head], q_recv.at[my_run], owner).start()

        @pl.when(owner == me)
        def _():
            qbuf[my_run] = part[...]

    for step in range(1, n):
        peer = lax.rem(me + step, n)
        cols = columns(peer // group)
        copy(k_ref.at[:, cols], kbuf.at[me], k_send.at[peer], k_recv.at[me], peer).start()
        copy(v_ref.at[:, cols], vbuf.at[me], v_send.at[peer], v_recv.at[me], peer).start()
    kbuf[me] = k_ref[:, columns(my_head)]
    vbuf[me] = v_ref[:, columns(my_head)]
    sbuf[me] = st_ref[me]

    for source in range(n):
        @pl.when(source != me)
        def _():
            arrived(sbuf.at[source], s_recv.at[source])

    decay = dec_ref[...]
    state = init_ref[...]
    for place in range(n):
        ebuf[place] = state.astype(ebuf.dtype)
        if place < n - 1:
            state = state * decay + sbuf[place].astype(jnp.float32)
    for step in range(1, n):
        peer = lax.rem(me + step, n)
        copy(ebuf.at[peer], ent.at[me], e_send.at[peer], e_recv.at[me], peer).start()
    ent[me] = ebuf[me]

    offset = off_ref[my_head] * LOG2E
    factor = width ** (-0.5) * LOG2E
    row_at = lax.broadcasted_iota(jnp.int32, (rows, rows), 0)
    col_at = lax.broadcasted_iota(jnp.int32, (rows, rows), 1)
    below = col_at < row_at
    later = jnp.where(below, 1.0, 0.0).astype(jnp.bfloat16)

    def tile(query, keys, shift, mask):
        score = (
            lax.dot_general(
                query, keys, (((1,), (1,)), ((), ())), preferred_element_type=jnp.float32
            ) * factor + shift
        )
        soft = jnp.maximum(score, 0.0) + jnp.log(1.0 + jnp.exp2(-jnp.abs(score))) * LOG2E
        take = score - soft
        if mask is not None:
            soft = jnp.where(mask, soft, 0.0)
        suffix = jnp.dot(soft.astype(jnp.bfloat16), later, preferred_element_type=jnp.float32)
        return take - suffix, suffix[:, 0:1] + soft[:, 0:1]

    def weigh(power, mask, values):
        weight = jnp.exp2(power)
        if mask is not None:
            weight = jnp.where(mask, weight, 0.0)
        return jnp.dot(weight.astype(jnp.bfloat16), values, preferred_element_type=jnp.float32)

    for run in range(heads):
        block = run * group + flip(run, my_slot)
        for source in range(run * group, (run + 1) * group):
            @pl.when(source != me)
            def _():
                arrived(kbuf.at[source], k_recv.at[source])
                arrived(vbuf.at[source], v_recv.at[source])

        @pl.when(block != me)
        def _():
            arrived(qbuf.at[run], q_recv.at[run])

        query = qbuf[run]
        power, before = tile(query, kbuf[block], offset, below)
        total = weigh(power, below, vbuf[block])

        def visit(index, carry):
            total, before = carry
            first = block - 1 - 2 * index
            second = jnp.maximum(first - 1, 0)
            shift = jnp.where(first >= 1, offset, -1e9)
            power_a, gone_a = tile(query, kbuf[first], offset, None)
            power_b, gone_b = tile(query, kbuf[second], shift, None)
            middle = before + gone_a
            total = total + weigh(power_a - before, None, vbuf[first])
            total = total + weigh(power_b - middle, None, vbuf[second])
            return total, middle + gone_b

        total, _unused = lax.fori_loop(0, (block + 1) // 2, visit, (total, before))
        res[run] = total.astype(res.dtype)

        @pl.when(block != me)
        def _():
            copy(res.at[run], back.at[my_head], r_send.at[run], r_recv.at[my_head], block).start()

        @pl.when(block == me)
        def _():
            back[my_head] = res[run]

    for source in range(n):
        @pl.when(source != me)
        def _():
            arrived(ent.at[source], e_recv.at[source])
    ent_ref[...] = ent[...]
    for head in range(heads):
        @pl.when(head * group + owner_slot != me)
        def _():
            arrived(back.at[head], r_recv.at[head])
        out_ref[:, head * width:(head + 1) * width] = back[head]

    for step in range(1, n):
        peer = lax.rem(me + step, n)
        cols = columns(peer // group)
        sent(st_ref.at[peer], s_send.at[peer])
        sent(ebuf.at[peer], e_send.at[peer])
        sent(k_ref.at[:, cols], k_send.at[peer])
        sent(v_ref.at[:, cols], v_send.at[peer])
    for head in range(heads):
        @pl.when(head * group + owner_slot != me)
        def _():
            sent(q_ref.at[:, head * width:(head + 1) * width], q_send.at[head])

        @pl.when(head * group + flip(head, my_slot) != me)
        def _():
            sent(res.at[head], r_send.at[head])


def mix(n, heads, offsets, query, key, value, state, first_state, decay):
    rows = query.shape[0]
    width = query.shape[1] // heads
    vmem = pl.BlockSpec(memory_space=pltpu.VMEM)
    half = jnp.bfloat16
    slab = state.shape[1:]
    return pl.pallas_call(
        functools.partial(mixer_kernel, n, heads),
        out_shape=(
            jax.ShapeDtypeStruct(query.shape, half),
            jax.ShapeDtypeStruct(state.shape, half),
        ),
        in_specs=[pl.BlockSpec(memory_space=pltpu.SMEM)] + [vmem] * 6,
        out_specs=(vmem, vmem),
        scratch_shapes=[
            pltpu.VMEM((n, rows, width), half),
            pltpu.VMEM((n, rows, width), half),
            pltpu.VMEM((heads, rows, width), half),
            pltpu.VMEM((heads, rows, width), half),
            pltpu.VMEM((heads, rows, width), half),
            pltpu.VMEM((n,) + slab, half),
            pltpu.VMEM((n,) + slab, half),
            pltpu.VMEM((n,) + slab, half),
            *(pltpu.SemaphoreType.DMA((size,)) for size in (n, n, heads, heads, n, n) * 2),
        ],
        compiler_params=pltpu.CompilerParams(
            collective_id=0, has_side_effects=True, vmem_limit_bytes=40 * 2**20
        ),
        cost_estimate=pl.CostEstimate(
            flops=4 * 10**9, bytes_accessed=8 * 10**6, transcendentals=6 * 10**6
        ),
    )(offsets, query, key, value, state, first_state, decay)


def rotate(values, positions):
    half_width = values.shape[-1] // 2
    inverse = rope_base ** (-jnp.arange(half_width, dtype=jnp.float32) / half_width)
    angles = positions.astype(jnp.float32)[:, None] * inverse[None, :]
    cosine = jnp.cos(angles)[:, None, :]
    sine_table = jnp.sin(angles)[:, None, :]
    first_half = values[..., :half_width]
    second_half = values[..., half_width:]
    return jnp.concatenate(
        [
            first_half * cosine - second_half * sine_table,
            second_half * cosine + first_half * sine_table,
        ],
        axis=-1,
    )


def body(
    inputs,
    input_gain,
    stick_query_w,
    stick_key_w,
    stick_value_w,
    ret_query_w,
    ret_key_w,
    ret_value_w,
    stick_offset,
    ret_log_decay,
    initial_state,
    stick_gain,
    ret_gain,
    stick_out_w,
    ret_out_w,
):
    tok_rows = inputs.shape[0]
    matrices = (stick_query_w, stick_key_w, stick_value_w, ret_query_w, ret_key_w, ret_value_w)
    packed = jnp.concatenate([inputs, jnp.broadcast_to(input_gain[None, :], (16, inputs.shape[1]))])
    gathered = lax.all_gather(packed, "tp", axis=1, tiled=True)
    wide = gathered[:tok_rows].astype(jnp.float32)
    squares = jnp.sum(jnp.square(wide), axis=1)
    scaled = (wide * gathered[tok_rows].astype(jnp.float32)[None, :]).astype(jnp.bfloat16)
    stick_out_w, ret_out_w, scaled = lax.optimization_barrier((stick_out_w, ret_out_w, scaled))
    projected = tuple(
        (jnp.dot(scaled, matrix, preferred_element_type=jnp.float32) for matrix in matrices)
    )
    row_scale = lax.rsqrt(squares / D + epsilon)
    stick_query, stick_key, stick_value, ret_query, ret_key, ret_value = tuple(
        ((running * row_scale[:, None]).astype(jnp.bfloat16) for running in projected)
    )
    head_count = stick_offset.shape[0]
    head_width = stick_query.shape[1] // head_count
    first_pos = lax.axis_index("sp") * tok_rows
    query_pos = first_pos + jnp.arange(tok_rows, dtype=jnp.int32)
    ret_heads = ret_log_decay.shape[0]
    ret_width = ret_query.shape[1] // ret_heads
    turned_query = rotate(
        ret_query.reshape(tok_rows, ret_heads, ret_width).astype(jnp.float32), query_pos
    )
    turned_key = rotate(
        ret_key.reshape(tok_rows, ret_heads, ret_width).astype(jnp.float32), query_pos
    ) * ret_width ** (-0.5)
    ret_values = ret_value.reshape(tok_rows, ret_heads, ret_width)
    local_pos = jnp.arange(tok_rows, dtype=jnp.float32)
    distance = local_pos[:, None] - local_pos[None, :]
    decay_mask = jnp.where(
        distance[None] >= 0.0,
        jnp.exp(ret_log_decay[:, None, None] * jnp.maximum(distance, 0.0)[None]),
        0.0,
    )
    half = jnp.bfloat16
    key_decay = jnp.exp(ret_log_decay[None, :] * (tok_rows - 1.0 - local_pos[:, None]))
    own_state = jnp.einsum(
        "shd,she->hde", (turned_key * key_decay[:, :, None]).astype(half), ret_values,
        preferred_element_type=jnp.float32,
    )
    count = lax.axis_size("sp")
    slab = ret_width // count
    block_decay = jnp.exp(ret_log_decay * tok_rows)
    state_parts = jnp.swapaxes(
        own_state.astype(half).reshape(ret_heads, count, slab, ret_width), 0, 1
    ).reshape(count, ret_heads * slab, ret_width)
    stick_out, entering_parts = mix(
        count, head_count, stick_offset, stick_query, stick_key, stick_value, state_parts,
        initial_state.reshape(ret_heads * slab, ret_width),
        jnp.broadcast_to(
            block_decay[:, None, None], (ret_heads, slab, ret_width)
        ).reshape(ret_heads * slab, ret_width),
    )
    entering = jnp.swapaxes(
        entering_parts.reshape(count, ret_heads, slab, ret_width), 0, 1
    ).reshape(ret_heads, ret_width, ret_width)
    turned_query, turned_key = turned_query.astype(half), turned_key.astype(half)
    scores = (
        jnp.einsum("thd,shd->hts", turned_query, turned_key, preferred_element_type=jnp.float32)
        * decay_mask
    ).astype(half)
    inner_part = jnp.einsum("hts,she->the", scores, ret_values, preferred_element_type=jnp.float32)
    query_decay = jnp.exp(ret_log_decay[None, :] * (local_pos[:, None] + 1.0))
    cross_part = (
        jnp.einsum("thd,hde->the", turned_query, entering, preferred_element_type=jnp.float32)
        * query_decay[:, :, None]
    )
    ret_total = inner_part + cross_part
    centered = ret_total - jnp.mean(ret_total, axis=2, keepdims=True)
    normed = centered * lax.rsqrt(jnp.mean(centered * centered, axis=2, keepdims=True) + epsilon)
    ret_normed = (normed.reshape(tok_rows, ret_heads * ret_width) * ret_gain).astype(jnp.bfloat16)
    stick_total = stick_out.astype(jnp.float32)
    stick_squares = lax.psum(jnp.sum(jnp.square(stick_total), axis=1), "tp")
    stick_scale = lax.rsqrt(stick_squares / (STICK_HEADS * STICK_DIM) + epsilon)
    stick_normed = (stick_total * stick_scale[:, None] * stick_gain).astype(jnp.bfloat16)
    stick_cols, ret_cols = (
        lax.all_gather(stick_out_w, "sp", axis=1, tiled=True),
        lax.all_gather(ret_out_w, "sp", axis=1, tiled=True),
    )
    stick_part = jnp.dot(stick_normed, stick_cols, preferred_element_type=jnp.float32)
    return lax.psum_scatter(
        (stick_part + jnp.dot(ret_normed, ret_cols, preferred_element_type=jnp.float32)).astype(
            jnp.bfloat16
        ),
        "tp",
        scatter_dimension=0,
        tiled=True,
    )


def solution(mesh):
    in_specs = (
        P("sp", "tp"),
        P("tp"),
        P(None, "tp"),
        P(None, "tp"),
        P(None, "tp"),
        P(None, "tp"),
        P(None, "tp"),
        P(None, "tp"),
        P("tp"),
        P("tp"),
        P("tp", "sp", None),
        P("tp"),
        P("tp"),
        P("tp", "sp"),
        P("tp", "sp"),
    )
    out_specs = P(("sp", "tp"), None)
    return jax.shard_map(body, mesh=mesh, in_specs=in_specs, out_specs=out_specs, check_vma=False)
```
